32 devices in a mesh: grp: 2 (over x), ep: 8 (over z, y), tp: 2 (over core).
Axes of the slice: x: 2, y: 2, z: 4, core: 2. Of those that a mesh axis runs over, the one named last changes fastest.
Arguments:
- tokens: bfloat16 [1024, 1024], P(('grp', 'ep')), parts along dimension 0, may hold values from -6 to 6
- routes: int32 [1024, 4], P(('grp', 'ep')), parts along dimension 0, may hold values from 0 to 7, all different within a row; in each aligned block of 64 rows (0 to 63, 64 to 127, ...) at most 64 rows name the same one
- gates: float32 [1024, 4], P(('grp', 'ep')), parts along dimension 0, may hold values from 0.05 to 1
- norm_gain: float32 [1024], replicated, may hold values from 0.1 to 1.9
- w_gate: bfloat16 [8, 1024, 1792], P('ep', None, 'tp'), may hold values from -0.1875 to 0.1875
- w_up: bfloat16 [8, 1024, 1792], P('ep', None, 'tp'), may hold values from -0.1875 to 0.1875
- w_down: bfloat16 [8, 1792, 1024], P('ep', 'tp'), may hold values from -0.125 to 0.125
Outputs:
- mixed: bfloat16 [1024, 1024], P(('grp', 'ep')), parts along dimension 0
The draws below stay inside these ranges and needn't reach their ends.
There are 2 independent parts, one for each index of `grp`. The reference program is written for one: setup_inputs(seed, part) draws one part's arguments, and reference() takes and returns one part's arrays. A program takes and returns all parts, laid end to end along the dimension named above; an argument that names none is the same for every part. Nothing has to cross between parts.
Inputs may be any that keep to these rules, and one draw needn't show every extreme that they name: `routes`: within the rows of one index of ep no expert is named more than 64 times; some expert is named exactly 64 times there in some or all of them.
All inputs are finite; a program needn't handle non-finite values.
Results may differ from the reference program's by a relative error of at most 0.0078.
Values may be sent and summed in bfloat16 or wider, within the bound.
A program may use at most 64 MiB of HBM per device.

```python
import math
import jax
import jax.numpy as jnp
import numpy as np
from jax import lax

D = 1024
FF = 1792
TOP_K = 4
TOK_DEV = 64
EXPERTS = 8
CAP = 64
TOKENS = 512
N_EP = 8
N_TP = 2


def steps_of(own_key, extent, pieces, low, high):
    factor_of = 1.0
    for axis_at, parts in pieces:
        heights = jax.random.uniform(jax.random.fold_in(jax.random.fold_in(own_key, 6), axis_at), (parts,), jnp.float32, low / len(pieces), high / len(pieces))
        factor_of = factor_of * jnp.repeat(jnp.exp(heights), extent[axis_at] // parts).reshape((-1,) + (1,) * (len(extent) - 1 - axis_at))
    return factor_of


def deal_out(rng, own, number, rows, count, top, bound, lean):
    ranking = jax.random.permutation(rng, count)
    packed, ordinary = shares(count, rows * top, bound, lean, True), shares(count, rows * top, bound, lean, False)
    places = jnp.arange(count)

    def named(lengths, turn):
        used = int((lengths > 0).sum())
        fixed = max(1, used // 4)
        shifted = fixed + (places - fixed + turn * (used - fixed)) % max(1, count - fixed)
        return jnp.zeros((count,), jnp.int32).at[ranking[jnp.where(places < fixed, places, shifted)]].set(jnp.asarray(lengths, jnp.int32))

    lengths = jnp.where(number % 4 == 0, named(packed, number // 4), named(ordinary, number - number // 4 - 1))
    mixed = jax.random.permutation(jax.random.fold_in(own, 3), count)
    donor, taker = mixed[0:count // 2 * 2:2], mixed[1:count // 2 * 2:2]
    room = jnp.minimum(lengths[donor] - 1, bound - lengths[taker]) // 2
    room = jnp.where((donor == ranking[0]) | (taker == ranking[0]) | (lengths[taker] == 0), 0, jnp.maximum(room, 0))
    shifted = jax.random.randint(jax.random.fold_in(own, 4), (count // 2,), 0, 1 << 20) % (room + 1)
    lengths = lengths.at[donor].add(-shifted).at[taker].add(shifted)
    members = jnp.searchsorted(jnp.cumsum(lengths), jnp.arange(rows * top), side="right").astype(jnp.int32)
    grid = members.reshape(top, rows).T
    grid = grid[jax.random.permutation(jax.random.fold_in(own, 1), rows)]
    turn = jax.random.randint(jax.random.fold_in(own, 2), (rows, 1), 0, top)
    return jnp.take_along_axis(grid, (jnp.arange(top)[None, :] + turn) % top, axis=1)


def shares(number_of, total, limit, skew, full):
    portions = [(1 << 20) // math.isqrt(rank ** skew) + 1 for rank in range(1, number_of + 1)]
    largest = limit if full else min(limit, max(-(-total // number_of), total * portions[0] // sum(portions)))
    least = 1 if total - largest >= number_of - 1 else 0
    given, rest = [largest] + [least] * (number_of - 1), total - largest - least * (number_of - 1)
    while rest > 0:
        movable = [i for i in range(1, number_of) if given[i] < largest] or [i for i in range(1, number_of) if given[i] < limit]
        mass, left = sum([portions[i] for i in movable]), rest
        for i in movable:
            extra = min(limit - given[i], max(1, left * portions[i] // mass), rest)
            given[i] = given[i] + extra
            rest = rest - extra
    return np.array(given)


def noise(key, extent, scale, bound, cuts=(), kind=jnp.bfloat16):
    entries = scale * jax.random.normal(key, extent, jnp.float32)
    if cuts:
        entries = entries * steps_of(key, extent, cuts, -0.22, 0.18)
    return jnp.clip(entries, -bound, bound).astype(kind)


def setup_inputs(seed: int = 0, part: int = 0) -> dict:
    streams_of = jax.random.split(jax.random.key(seed), 8)
    part_splits = jax.random.split(jax.random.fold_in(streams_of[7], part), 8)
    tokens = noise(part_splits[0], (TOKENS, D), 1.0, 6.0, ((0, 8),))
    routes_keys = jax.random.split(jax.random.fold_in(part_splits[1], 1), TOKENS // TOK_DEV)
    routes_turns = jax.random.permutation(jax.random.fold_in(part_splits[1], 3), TOKENS // TOK_DEV)
    routes = jax.vmap(lambda own, number: deal_out(jax.random.fold_in(part_splits[1], 2), own, number, TOK_DEV, EXPERTS, TOP_K, CAP, 2))(routes_keys, routes_turns).reshape((TOKENS, TOP_K))
    gates = jnp.clip(0.05 + 0.95 * jax.random.uniform(part_splits[2], (TOKENS, TOP_K), jnp.float32) ** steps_of(part_splits[2], (TOKENS, TOP_K), ((0, 8),), -0.2, 0.2), 0.05, 1.0)
    norm_gain = jnp.clip(1.0 + 0.18 * jax.random.normal(streams_of[3], (D,), jnp.float32), 0.1, 1.9)
    w_gate = noise(streams_of[4], (EXPERTS, D, FF), D ** -0.5, 0.1875, ((0, 8), (2, 2)))
    w_up = noise(streams_of[5], (EXPERTS, D, FF), D ** -0.5, 0.1875, ((0, 8), (2, 2)))
    w_down = noise(streams_of[6], (EXPERTS, FF, D), FF ** -0.5, 0.125, ((0, 8), (1, 2)))
    return {"tokens": tokens, "routes": routes, "gates": gates, "norm_gain": norm_gain, "w_gate": w_gate, "w_up": w_up, "w_down": w_down}


EPS = 1e-06

def reference(tokens, routes, gates, norm_gain, w_gate, w_up, w_down):
    xf = tokens.astype(jnp.float32)
    normed = (xf * lax.rsqrt(lax.optimization_barrier(jnp.mean(xf * xf, axis=-1, keepdims=True)) + EPS) * norm_gain.astype(jnp.float32)).astype(jnp.bfloat16)
    flat = routes.reshape(-1).astype(jnp.int32)
    pair_count = TOKENS * TOP_K
    rows_max = N_EP * CAP
    block = FF // N_TP

    def expert(index):
        chosen = jnp.nonzero(flat == index, size=rows_max, fill_value=pair_count)[0].astype(jnp.int32)
        source = jnp.minimum(chosen // TOP_K, TOKENS - 1).astype(jnp.int32)
        picked = jnp.take(normed, source, axis=0)
        gate_act = jnp.dot(picked, w_gate[index], preferred_element_type=jnp.float32)
        up_act = jnp.dot(picked, w_up[index], preferred_element_type=jnp.float32)
        hidden = (jax.nn.silu(gate_act) * up_act).astype(jnp.bfloat16)
        total = jnp.zeros((rows_max, D), jnp.float32)
        for part_index in range(N_TP):
            rows_down = w_down[index, part_index * block:(part_index + 1) * block]
            part = jnp.dot(hidden[:, part_index * block:(part_index + 1) * block], rows_down, preferred_element_type=jnp.float32).astype(jnp.bfloat16)
            total = total + lax.optimization_barrier(part).astype(jnp.float32)
        return (chosen, total.astype(jnp.bfloat16))
    chosen_all, results_all = lax.map(expert, jnp.arange(EXPERTS, dtype=jnp.int32))
    pair_out = jnp.zeros((pair_count, D), jnp.bfloat16).at[chosen_all.reshape(-1)].set(results_all.reshape(-1, D), mode='drop')
    mixed = lax.optimization_barrier(jnp.sum(gates.astype(jnp.float32)[:, :, None] * pair_out.reshape(TOKENS, TOP_K, D).astype(jnp.float32), axis=1))
    return mixed.astype(jnp.bfloat16)
```

```python
import functools

import jax
import jax.numpy as jnp
from jax import lax
from jax.experimental import pallas as pl
from jax.experimental.pallas import tpu as pltpu
from jax.sharding import PartitionSpec as P

EPS = 1e-06
MESH = pl.DeviceIdType.MESH


def flipped(value, bits):
    result, bit = value, 1
    while bit <= bits:
        if bits & bit:
            result = result + bit - 2 * bit * ((value // bit) % 2)
        bit *= 2
    return result


def dense_kernel(
    lines, tok_ref, route_ref, gate_ref, gain_ref, wg_hbm, wu_hbm, wd_hbm, out_ref,
    wg, wu, wd, xg, gg, po, rd, ys, ry, zs, rz, keep, fin, ro,
    w_sem, zx_s, zx_r, zg_s, zg_r, yx_s, yx_r, yg_s, yg_r, dx_s, dx_r,
    rd_s, rd_r, ry_s, ry_r, rz_s, rz_r, ro_s, ro_r,
):
    rows, width = tok_ref.shape
    half = rows // 2
    grp, me, lane = lax.axis_index("grp"), lax.axis_index("ep"), lax.axis_index("tp")
    line, col = me // 2, me % 2
    peer_z = [(grp, flipped(line, k) * 2 + col, lane) for k in range(lines)]
    peer_y = (grp, line * 2 + 1 - col, lane)
    peer_c = (grp, me, 1 - lane)
    sent = []

    weights = [
        pltpu.make_async_copy(src.at[0], dst, w_sem.at[i])
        for i, (src, dst) in enumerate(((wg_hbm, wg), (wu_hbm, wu), (wd_hbm, wd)))
    ]
    for copy in weights:
        copy.start()
    barrier = pltpu.get_barrier_semaphore()
    others = peer_z[1:] + [peer_y, peer_c]
    for other in others:
        pl.semaphore_signal(barrier, inc=1, device_id=other, device_id_type=MESH)

    def remote(src, dst, send_sem, recv_sem, device):
        copy = pltpu.make_async_remote_copy(
            src_ref=src, dst_ref=dst, send_sem=send_sem, recv_sem=recv_sem,
            device_id=device, device_id_type=MESH,
        )
        copy.start()
        sent.append(copy)

    def landed(ref, sem):
        pltpu.make_async_remote_copy(
            src_ref=ref, dst_ref=ref, send_sem=sem, recv_sem=sem,
            device_id=peer_c, device_id_type=MESH,
        ).wait_recv()

    gain = gain_ref[...]
    for part, first in ((0, lane * half), (1, (1 - lane) * half)):
        xf = tok_ref[pl.ds(pl.multiple_of(first, half), half), :].astype(jnp.float32)
        scale = lax.rsqrt(jnp.mean(xf * xf, axis=-1, keepdims=True) + EPS)
        xg[0, part, 0] = (xf * scale * gain).astype(jnp.bfloat16)
    pieces = []
    for first in (lane * half, (1 - lane) * half):
        window = pl.ds(pl.multiple_of(first, half), half)
        names, scales = route_ref[window, :], gate_ref[window, :]
        expert = lax.broadcasted_iota(jnp.int32, (half, 2 * rows), 1)
        piece = jnp.zeros((half, 2 * rows), jnp.float32)
        for k in range(names.shape[1]):
            piece = piece + jnp.where(names[:, k:k + 1] == expert, scales[:, k:k + 1], 0.0)
        pieces.append(piece)
    table = jnp.concatenate(pieces + pieces, axis=0)
    gg[0, 0] = jnp.transpose(table)[: gg.shape[2]]

    pl.semaphore_wait(barrier, len(others))

    def over_y(k):
        remote(xg.at[k, 0, 0], xg.at[k, 0, 1], yx_s.at[k], yx_r.at[k], peer_y)
        remote(gg.at[k, 0], gg.at[k, 1], yg_s.at[k], yg_r.at[k], peer_y)

    def over_c(k, j):
        remote(xg.at[k, 0, j], xg.at[k, 1, j], dx_s.at[k, j], dx_r.at[k, j], peer_c)

    over_y(0)
    for k in range(1, lines):
        remote(xg.at[0, 0, 0], xg.at[k, 0, 0], zx_s.at[k], zx_r.at[k], peer_z[k])
        remote(gg.at[0, 0], gg.at[k, 0], zg_s.at[k], zg_r.at[k], peer_z[k])

    def from_z(k):
        landed(xg.at[k, 0, 0], zx_r.at[k])
        landed(gg.at[k, 0], zg_r.at[k])
        over_y(k)
        over_c(k, 0)

    def from_y(k):
        landed(xg.at[k, 0, 1], yx_r.at[k])
        landed(gg.at[k, 1], yg_r.at[k])
        over_c(k, 1)

    def compute(k):
        if k:
            landed(xg.at[k, 1, 0], dx_r.at[k, 0])
        landed(xg.at[k, 1, 1], dx_r.at[k, 1])
        if k == 0:
            weights[0].wait()
            weights[1].wait()
        count = 2 * rows
        x = xg[k].reshape(count, width)
        spot = lax.broadcasted_iota(jnp.int32, gg.shape[2:], 1)
        first, second = gg[k, 0], gg[k, 1]
        mine = lax.broadcasted_iota(jnp.int32, gg.shape[2:], 0) == me
        row_a = jnp.sum(jnp.where(mine, first, 0.0), axis=0, keepdims=True)
        row_b = jnp.sum(jnp.where(mine, second, 0.0), axis=0, keepdims=True)
        at = lax.broadcasted_iota(jnp.int32, (count, count), 0)
        token = (at // rows) * half + at % half
        hit = lax.broadcasted_iota(jnp.int32, (count, count), 1) == token
        column = (at // half) % 2
        gate = jnp.sum(
            jnp.where(hit, jnp.where(column == 0, row_a, row_b), 0.0), axis=1, keepdims=True
        )
        g = jnp.dot(x, wg[...], preferred_element_type=jnp.float32)
        u = jnp.dot(x, wu[...], preferred_element_type=jnp.float32)
        hidden = (g / (1.0 + jnp.exp(-g)) * u * gate).astype(jnp.bfloat16)
        if k == 0:
            weights[2].wait()
        y = jnp.dot(hidden, wd[...], preferred_element_type=jnp.float32)
        po[k] = y.astype(jnp.bfloat16).reshape(2, 2, half, width)
        remote(po.at[k, 1], rd.at[k], rd_s.at[k], rd_r.at[k], peer_c)

    def back_y(k):
        landed(rd.at[k], rd_r.at[k])
        ys[k] = (po[k, 0, 1].astype(jnp.float32) + rd[k, 1].astype(jnp.float32)).astype(jnp.bfloat16)
        remote(ys.at[k], ry.at[k], ry_s.at[k], ry_r.at[k], peer_y)

    def back_z(k):
        landed(ry.at[k], ry_r.at[k])
        total = (
            po[k, 0, 0].astype(jnp.float32)
            + rd[k, 0].astype(jnp.float32)
            + ry[k].astype(jnp.float32)
        )
        if k == 0:
            keep[...] = total
        else:
            zs[k] = total.astype(jnp.bfloat16)
            remote(zs.at[k], rz.at[k], rz_s.at[k], rz_r.at[k], peer_z[k])

    def step(fn, k, low=0):
        if low <= k < lines:
            fn(k)

    for tick in range(lines + 3):
        step(from_z, tick + 1, 1)
        step(from_y, tick)
        step(compute, tick - 1)
        step(back_y, tick - 2)
        step(back_z, tick - 3)
    total = keep[...]
    for k in range(1, lines):
        landed(rz.at[k], rz_r.at[k])
        total = total + rz[k].astype(jnp.float32)
    fin[...] = total.astype(jnp.bfloat16)
    remote(fin, ro, ro_s, ro_r, peer_c)
    out_ref[pl.ds(pl.multiple_of(lane * half, half), half), :] = fin[...]
    landed(ro, ro_r)
    out_ref[pl.ds(pl.multiple_of((1 - lane) * half, half), half), :] = ro[...]
    for copy in sent:
        copy.wait_send()


def dense_device(lines, tokens, routes, gates, norm_gain, w_gate, w_up, w_down):
    rows, width = tokens.shape
    half = rows // 2
    units = w_gate.shape[2]
    experts = lines * 2
    bf16, f32 = jnp.bfloat16, jnp.float32
    dma = pltpu.SemaphoreType.DMA
    vmem, anywhere = pl.BlockSpec(memory_space=pltpu.VMEM), pl.BlockSpec(memory_space=pl.ANY)
    return pl.pallas_call(
        functools.partial(dense_kernel, lines),
        out_shape=jax.ShapeDtypeStruct((rows, width), bf16),
        in_specs=[vmem] * 4 + [anywhere] * 3,
        out_specs=vmem,
        scratch_shapes=[
            pltpu.VMEM((width, units), bf16),
            pltpu.VMEM((width, units), bf16),
            pltpu.VMEM((units, width), bf16),
            pltpu.VMEM((lines, 2, 2, half, width), bf16),
            pltpu.VMEM((lines, 2, experts, 2 * rows), f32),
            pltpu.VMEM((lines, 2, 2, half, width), bf16),
            pltpu.VMEM((lines, 2, half, width), bf16),
            pltpu.VMEM((lines, half, width), bf16),
            pltpu.VMEM((lines, half, width), bf16),
            pltpu.VMEM((lines, half, width), bf16),
            pltpu.VMEM((lines, half, width), bf16),
            pltpu.VMEM((half, width), f32),
            pltpu.VMEM((half, width), bf16),
            pltpu.VMEM((half, width), bf16),
            dma((3,)),
            dma((lines,)), dma((lines,)), dma((lines,)), dma((lines,)),
            dma((lines,)), dma((lines,)), dma((lines,)), dma((lines,)),
            dma((lines, 2)), dma((lines, 2)),
            dma((lines,)), dma((lines,)), dma((lines,)), dma((lines,)),
            dma((lines,)), dma((lines,)), dma, dma,
        ],
        compiler_params=pltpu.CompilerParams(collective_id=0, has_side_effects=True),
    )(tokens, routes, gates, norm_gain.reshape(1, width), w_gate, w_up, w_down)


def packed_device(tokens, routes, gates, norm_gain, w_gate, w_up, w_down):
    tok_rows, width = tokens.shape
    top = routes.shape[1]
    ep_count = lax.axis_size("ep")
    tp_count = lax.axis_size("tp")
    capacity = max(2, min(tok_rows, 3 * tok_rows * top // ep_count))
    share = width // tp_count
    lane = lax.axis_index("tp")
    xf = tokens.astype(jnp.float32)
    normed = (xf * lax.rsqrt(jnp.mean(xf * xf, axis=-1, keepdims=True) + EPS) * norm_gain).astype(
        jnp.bfloat16
    )
    flat = routes.reshape(-1)
    onehot = (flat[:, None] == jnp.arange(ep_count, dtype=jnp.int32)[None, :]).astype(jnp.int32)
    earlier = jnp.cumsum(onehot, axis=0) - onehot
    rank = jnp.sum(earlier * onehot, axis=1)
    slot = flat * capacity + rank
    placing = (jnp.arange(ep_count * capacity, dtype=jnp.int32)[:, None] == slot[None, :]).astype(
        jnp.bfloat16
    )
    repeated = jnp.repeat(normed, top, axis=0)
    outgoing = jnp.dot(placing, repeated, preferred_element_type=jnp.float32).astype(jnp.bfloat16)
    outgoing = outgoing.reshape(ep_count, capacity, width)
    mine = lax.dynamic_slice_in_dim(outgoing, lane * share, share, 2)
    full = lax.all_gather(
        lax.all_to_all(mine, "ep", split_axis=0, concat_axis=0, tiled=True),
        "tp",
        axis=2,
        tiled=True,
    )
    sources = full.shape[0]
    items = full.shape[1]
    rows = full.reshape(sources * items, width)
    gate_act = jnp.dot(rows, w_gate[0], preferred_element_type=jnp.float32)
    up_act = jnp.dot(rows, w_up[0], preferred_element_type=jnp.float32)
    hidden = (jax.nn.silu(gate_act) * up_act).astype(jnp.bfloat16)
    partial_value = jnp.dot(hidden, w_down[0], preferred_element_type=jnp.float32).astype(
        jnp.bfloat16
    )
    summed = lax.psum_scatter(
        lax.optimization_barrier(partial_value)
        .astype(jnp.float32)
        .reshape(sources, items, width)
        .astype(jnp.bfloat16),
        "tp",
        scatter_dimension=2,
        tiled=True,
    )
    returned = lax.all_to_all(summed, "ep", split_axis=0, concat_axis=0, tiled=True)
    back = returned.reshape(ep_count * capacity, returned.shape[2])
    picked = jnp.take(back, slot, axis=0).reshape(tok_rows, top, back.shape[1])
    mixed = jnp.sum(gates[:, :, None] * picked.astype(jnp.float32), axis=1).astype(jnp.bfloat16)
    mixed = lax.all_gather(mixed, "tp", axis=1, tiled=True)
    return mixed


def per_device(tokens, routes, gates, norm_gain, w_gate, w_up, w_down):
    rows, width = tokens.shape
    ep_count, tp_count = lax.axis_size("ep"), lax.axis_size("tp")
    lines = ep_count // 2
    whole = 3 * rows * routes.shape[1] // ep_count >= rows
    fits = lines >= 2 and lines & (lines - 1) == 0 and lines * 2 == ep_count and ep_count % 8 == 0
    if whole and fits and tp_count == 2 and rows % 64 == 0 and width % 128 == 0:
        return dense_device(lines, tokens, routes, gates, norm_gain, w_gate, w_up, w_down)
    return packed_device(tokens, routes, gates, norm_gain, w_gate, w_up, w_down)


def solution(mesh):
    return jax.shard_map(
        per_device,
        mesh=mesh,
        in_specs=(
            P(("grp", "ep"), None),
            P(("grp", "ep"), None),
            P(("grp", "ep"), None),
            P(),
            P("ep", None, "tp"),
            P("ep", None, "tp"),
            P("ep", "tp", None),
        ),
        out_specs=P(("grp", "ep"), None),
        check_vma=False,
    )
```

```python
import functools

import jax
import jax.numpy as jnp
from jax import lax
from jax.experimental import pallas as pl
from jax.experimental.pallas import tpu as pltpu
from jax.sharding import PartitionSpec as P

EPS = 1e-06
MESH = pl.DeviceIdType.MESH


def flipped(value, bits):
    result, bit = value, 1
    while bit <= bits:
        if bits & bit:
            result = result + bit - 2 * bit * ((value // bit) % 2)
        bit *= 2
    return result


def dense_kernel(
    lines, tok_ref, route_ref, gate_ref, gain_ref, wg_hbm, wu_hbm, wd_hbm, out_ref,
    wg, wu, wd, xg, gg, po, rd, ys, ry, zs, rz, keep, fin, ro,
    w_sem, zx_s, zx_r, zg_s, zg_r, yx_s, yx_r, yg_s, yg_r, dx_s, dx_r,
    rd_s, rd_r, ry_s, ry_r, rz_s, rz_r, ro_s, ro_r,
):
    rows, width = tok_ref.shape
    half = rows // 2
    grp, me, lane = lax.axis_index("grp"), lax.axis_index("ep"), lax.axis_index("tp")
    line, col = me // 2, me % 2
    peer_z = [(grp, flipped(line, k) * 2 + col, lane) for k in range(lines)]
    peer_y = (grp, line * 2 + 1 - col, lane)
    peer_c = (grp, me, 1 - lane)
    sent = []

    weights = [
        pltpu.make_async_copy(src.at[0], dst, w_sem.at[i])
        for i, (src, dst) in enumerate(((wg_hbm, wg), (wu_hbm, wu), (wd_hbm, wd)))
    ]
    for copy in weights:
        copy.start()
    barrier = pltpu.get_barrier_semaphore()
    others = peer_z[1:] + [peer_y, peer_c]
    for other in others:
        pl.semaphore_signal(barrier, inc=1, device_id=other, device_id_type=MESH)

    def remote(src, dst, send_sem, recv_sem, device):
        copy = pltpu.make_async_remote_copy(
            src_ref=src, dst_ref=dst, send_sem=send_sem, recv_sem=recv_sem,
            device_id=device, device_id_type=MESH,
        )
        copy.start()
        sent.append(copy)

    def landed(ref, sem):
        pltpu.make_async_remote_copy(
            src_ref=ref, dst_ref=ref, send_sem=sem, recv_sem=sem,
            device_id=peer_c, device_id_type=MESH,
        ).wait_recv()

    gain = gain_ref[...]
    for part, first in ((0, lane * half), (1, (1 - lane) * half)):
        xf = tok_ref[pl.ds(pl.multiple_of(first, half), half), :].astype(jnp.float32)
        scale = lax.rsqrt(jnp.mean(xf * xf, axis=-1, keepdims=True) + EPS)
        xg[0, part, 0] = (xf * scale * gain).astype(jnp.bfloat16)
    names, scales = route_ref[...], gate_ref[...]
    expert = lax.broadcasted_iota(jnp.int32, (gg.shape[2], rows), 0)
    table = jnp.zeros((gg.shape[2], rows), jnp.float32)
    for k in range(names.shape[0]):
        table = table + jnp.where(names[k:k + 1] == expert, scales[k:k + 1], 0.0)
    upper = jnp.concatenate([table[:, half:], table[:, :half]], axis=1)
    table = jnp.where(lane == 0, table, upper)
    gg[0, 0] = jnp.concatenate([table, table], axis=1)

    pl.semaphore_wait(barrier, len(others))

    def over_y(k):
        remote(xg.at[k, 0, 0], xg.at[k, 0, 1], yx_s.at[k], yx_r.at[k], peer_y)
        remote(gg.at[k, 0], gg.at[k, 1], yg_s.at[k], yg_r.at[k], peer_y)

    def over_c(k, j):
        remote(xg.at[k, 0, j], xg.at[k, 1, j], dx_s.at[k, j], dx_r.at[k, j], peer_c)

    over_y(0)
    for k in range(1, lines):
        remote(xg.at[0, 0, 0], xg.at[k, 0, 0], zx_s.at[k], zx_r.at[k], peer_z[k])
        remote(gg.at[0, 0], gg.at[k, 0], zg_s.at[k], zg_r.at[k], peer_z[k])

    def from_z(k):
        landed(xg.at[k, 0, 0], zx_r.at[k])
        landed(gg.at[k, 0], zg_r.at[k])
        over_y(k)
        over_c(k, 0)

    def from_y(k):
        landed(xg.at[k, 0, 1], yx_r.at[k])
        landed(gg.at[k, 1], yg_r.at[k])
        over_c(k, 1)

    def compute(k):
        if k:
            landed(xg.at[k, 1, 0], dx_r.at[k, 0])
        landed(xg.at[k, 1, 1], dx_r.at[k, 1])
        if k == 0:
            weights[0].wait()
            weights[1].wait()
        count = 2 * rows
        x = xg[k].reshape(count, width)
        spot = lax.broadcasted_iota(jnp.int32, gg.shape[2:], 1)
        first, second = gg[k, 0], gg[k, 1]
        mine = lax.broadcasted_iota(jnp.int32, gg.shape[2:], 0) == me
        row_a = jnp.sum(jnp.where(mine, first, 0.0), axis=0, keepdims=True)
        row_b = jnp.sum(jnp.where(mine, second, 0.0), axis=0, keepdims=True)
        at = lax.broadcasted_iota(jnp.int32, (count, count), 0)
        token = (at // rows) * half + at % half
        hit = lax.broadcasted_iota(jnp.int32, (count, count), 1) == token
        column = (at // half) % 2
        gate = jnp.sum(
            jnp.where(hit, jnp.where(column == 0, row_a, row_b), 0.0), axis=1, keepdims=True
        )
        g = jnp.dot(x, wg[...], preferred_element_type=jnp.float32)
        u = jnp.dot(x, wu[...], preferred_element_type=jnp.float32)
        hidden = (g / (1.0 + jnp.exp(-g)) * u * gate).astype(jnp.bfloat16)
        if k == 0:
            weights[2].wait()
        y = jnp.dot(hidden, wd[...], preferred_element_type=jnp.float32)
        po[k] = y.astype(jnp.bfloat16).reshape(2, 2, half, width)
        remote(po.at[k, 1], rd.at[k], rd_s.at[k], rd_r.at[k], peer_c)

    def back_y(k):
        landed(rd.at[k], rd_r.at[k])
        ys[k] = (po[k, 0, 1].astype(jnp.float32) + rd[k, 1].astype(jnp.float32)).astype(jnp.bfloat16)
        remote(ys.at[k], ry.at[k], ry_s.at[k], ry_r.at[k], peer_y)

    def back_z(k):
        landed(ry.at[k], ry_r.at[k])
        total = (
            po[k, 0, 0].astype(jnp.float32)
            + rd[k, 0].astype(jnp.float32)
            + ry[k].astype(jnp.float32)
        )
        if k == 0:
            keep[...] = total
        else:
            zs[k] = total.astype(jnp.bfloat16)
            remote(zs.at[k], rz.at[k], rz_s.at[k], rz_r.at[k], peer_z[k])

    def step(fn, k, low=0):
        if low <= k < lines:
            fn(k)

    for tick in range(lines + 3):
        step(from_z, tick + 1, 1)
        step(from_y, tick)
        step(compute, tick - 1)
        step(back_y, tick - 2)
        step(back_z, tick - 3)
    total = keep[...]
    for k in range(1, lines):
        landed(rz.at[k], rz_r.at[k])
        total = total + rz[k].astype(jnp.float32)
    fin[...] = total.astype(jnp.bfloat16)
    remote(fin, ro, ro_s, ro_r, peer_c)
    out_ref[pl.ds(pl.multiple_of(lane * half, half), half), :] = fin[...]
    landed(ro, ro_r)
    out_ref[pl.ds(pl.multiple_of((1 - lane) * half, half), half), :] = ro[...]
    for copy in sent:
        copy.wait_send()


def dense_device(lines, tokens, routes, gates, norm_gain, w_gate, w_up, w_down):
    rows, width = tokens.shape
    half = rows // 2
    units = w_gate.shape[2]
    experts = lines * 2
    bf16, f32 = jnp.bfloat16, jnp.float32
    dma = pltpu.SemaphoreType.DMA
    vmem, anywhere = pl.BlockSpec(memory_space=pltpu.VMEM), pl.BlockSpec(memory_space=pl.ANY)
    return pl.pallas_call(
        functools.partial(dense_kernel, lines),
        out_shape=pltpu.VMEM((rows, width), bf16),
        in_specs=[vmem] * 4 + [anywhere] * 3,
        out_specs=vmem,
        scratch_shapes=[
            pltpu.VMEM((width, units), bf16),
            pltpu.VMEM((width, units), bf16),
            pltpu.VMEM((units, width), bf16),
            pltpu.VMEM((lines, 2, 2, half, width), bf16),
            pltpu.VMEM((lines, 2, experts, 2 * rows), f32),
            pltpu.VMEM((lines, 2, 2, half, width), bf16),
            pltpu.VMEM((lines, 2, half, width), bf16),
            pltpu.VMEM((lines, half, width), bf16),
            pltpu.VMEM((lines, half, width), bf16),
            pltpu.VMEM((lines, half, width), bf16),
            pltpu.VMEM((lines, half, width), bf16),
            pltpu.VMEM((half, width), f32),
            pltpu.VMEM((half, width), bf16),
            pltpu.VMEM((half, width), bf16),
            dma((3,)),
            dma((lines,)), dma((lines,)), dma((lines,)), dma((lines,)),
            dma((lines,)), dma((lines,)), dma((lines,)), dma((lines,)),
            dma((lines, 2)), dma((lines, 2)),
            dma((lines,)), dma((lines,)), dma((lines,)), dma((lines,)),
            dma((lines,)), dma((lines,)), dma, dma,
        ],
        compiler_params=pltpu.CompilerParams(collective_id=0, has_side_effects=True),
    )(tokens, routes.T, gates.T, norm_gain.reshape(1, width), w_gate, w_up, w_down)


def packed_device(tokens, routes, gates, norm_gain, w_gate, w_up, w_down):
    tok_rows, width = tokens.shape
    top = routes.shape[1]
    ep_count = lax.axis_size("ep")
    tp_count = lax.axis_size("tp")
    capacity = max(2, min(tok_rows, 3 * tok_rows * top // ep_count))
    share = width // tp_count
    lane = lax.axis_index("tp")
    xf = tokens.astype(jnp.float32)
    normed = (xf * lax.rsqrt(jnp.mean(xf * xf, axis=-1, keepdims=True) + EPS) * norm_gain).astype(
        jnp.bfloat16
    )
    flat = routes.reshape(-1)
    onehot = (flat[:, None] == jnp.arange(ep_count, dtype=jnp.int32)[None, :]).astype(jnp.int32)
    earlier = jnp.cumsum(onehot, axis=0) - onehot
    rank = jnp.sum(earlier * onehot, axis=1)
    slot = flat * capacity + rank
    placing = (jnp.arange(ep_count * capacity, dtype=jnp.int32)[:, None] == slot[None, :]).astype(
        jnp.bfloat16
    )
    repeated = jnp.repeat(normed, top, axis=0)
    outgoing = jnp.dot(placing, repeated, preferred_element_type=jnp.float32).astype(jnp.bfloat16)
    outgoing = outgoing.reshape(ep_count, capacity, width)
    mine = lax.dynamic_slice_in_dim(outgoing, lane * share, share, 2)
    full = lax.all_gather(
        lax.all_to_all(mine, "ep", split_axis=0, concat_axis=0, tiled=True),
        "tp",
        axis=2,
        tiled=True,
    )
    sources = full.shape[0]
    items = full.shape[1]
    rows = full.reshape(sources * items, width)
    gate_act = jnp.dot(rows, w_gate[0], preferred_element_type=jnp.float32)
    up_act = jnp.dot(rows, w_up[0], preferred_element_type=jnp.float32)
    hidden = (jax.nn.silu(gate_act) * up_act).astype(jnp.bfloat16)
    partial_value = jnp.dot(hidden, w_down[0], preferred_element_type=jnp.float32).astype(
        jnp.bfloat16
    )
    summed = lax.psum_scatter(
        lax.optimization_barrier(partial_value)
        .astype(jnp.float32)
        .reshape(sources, items, width)
        .astype(jnp.bfloat16),
        "tp",
        scatter_dimension=2,
        tiled=True,
    )
    returned = lax.all_to_all(summed, "ep", split_axis=0, concat_axis=0, tiled=True)
    back = returned.reshape(ep_count * capacity, returned.shape[2])
    picked = jnp.take(back, slot, axis=0).reshape(tok_rows, top, back.shape[1])
    mixed = jnp.sum(gates[:, :, None] * picked.astype(jnp.float32), axis=1).astype(jnp.bfloat16)
    mixed = lax.all_gather(mixed, "tp", axis=1, tiled=True)
    return mixed


def per_device(tokens, routes, gates, norm_gain, w_gate, w_up, w_down):
    rows, width = tokens.shape
    ep_count, tp_count = lax.axis_size("ep"), lax.axis_size("tp")
    lines = ep_count // 2
    whole = 3 * rows * routes.shape[1] // ep_count >= rows
    fits = lines >= 2 and lines & (lines - 1) == 0 and lines * 2 == ep_count and ep_count % 8 == 0
    if whole and fits and tp_count == 2 and rows % 64 == 0 and width % 128 == 0:
        return dense_device(lines, tokens, routes, gates, norm_gain, w_gate, w_up, w_down)
    return packed_device(tokens, routes, gates, norm_gain, w_gate, w_up, w_down)


def solution(mesh):
    return jax.shard_map(
        per_device,
        mesh=mesh,
        in_specs=(
            P(("grp", "ep"), None),
            P(("grp", "ep"), None),
            P(("grp", "ep"), None),
            P(),
            P("ep", None, "tp"),
            P("ep", None, "tp"),
            P("ep", "tp", None),
        ),
        out_specs=P(("grp", "ep"), None),
        check_vma=False,
    )
```

```python
import functools

import jax
import jax.numpy as jnp
from jax import lax
from jax.experimental import pallas as pl
from jax.experimental.pallas import tpu as pltpu
from jax.sharding import PartitionSpec as P

EPS = 1e-06
MESH = pl.DeviceIdType.MESH
PIECES = 1


def flipped(value, bits):
    result, bit = value, 1
    while bit <= bits:
        if bits & bit:
            result = result + bit - 2 * bit * ((value // bit) % 2)
        bit *= 2
    return result


def dense_kernel(
    lines, tok_ref, route_ref, gate_ref, gain_ref, wg_hbm, wu_hbm, wd_hbm, out_ref,
    wg, wu, wd, xg, gg, po, rd, ys, ry, zs, rz, keep, fin, ro,
    w_sem, zx_s, zx_r, zg_s, zg_r, yx_s, yx_r, yg_s, yg_r, dx_s, dx_r,
    rd_s, rd_r, ry_s, ry_r, rz_s, rz_r, ro_s, ro_r,
):
    rows, width = tok_ref.shape
    half = rows // 2
    grp, me, lane = lax.axis_index("grp"), lax.axis_index("ep"), lax.axis_index("tp")
    line, col = me // 2, me % 2
    peer_z = [(grp, flipped(line, k) * 2 + col, lane) for k in range(lines)]
    peer_y = (grp, line * 2 + 1 - col, lane)
    peer_c = (grp, me, 1 - lane)
    sent = []

    weights = [
        pltpu.make_async_copy(src.at[0], dst, w_sem.at[i])
        for i, (src, dst) in enumerate(((wg_hbm, wg), (wu_hbm, wu), (wd_hbm, wd)))
    ]
    for copy in weights:
        copy.start()
    barrier = pltpu.get_barrier_semaphore()
    others = [peer_z[k] for k in range(1, lines) if k & (k - 1) == 0] + [peer_y, peer_c]
    for other in others:
        pl.semaphore_signal(barrier, inc=1, device_id=other, device_id_type=MESH)

    def remote(src, dst, send_sem, recv_sem, device):
        copy = pltpu.make_async_remote_copy(
            src_ref=src, dst_ref=dst, send_sem=send_sem, recv_sem=recv_sem,
            device_id=device, device_id_type=MESH,
        )
        copy.start()
        sent.append(copy)

    def landed(ref, sem):
        pltpu.make_async_remote_copy(
            src_ref=ref, dst_ref=ref, send_sem=sem, recv_sem=sem,
            device_id=peer_c, device_id_type=MESH,
        ).wait_recv()

    gain = gain_ref[...]
    for part, first in ((0, lane * half), (1, (1 - lane) * half)):
        xf = tok_ref[pl.ds(pl.multiple_of(first, half), half), :].astype(jnp.float32)
        scale = lax.rsqrt(jnp.mean(xf * xf, axis=-1, keepdims=True) + EPS)
        xg[0, part, 0] = (xf * scale * gain).astype(jnp.bfloat16)
    names, scales = route_ref[...], gate_ref[...]
    expert = lax.broadcasted_iota(jnp.int32, (gg.shape[2], rows), 0)
    table = jnp.zeros((gg.shape[2], rows), jnp.float32)
    for k in range(names.shape[0]):
        table = table + jnp.where(names[k:k + 1] == expert, scales[k:k + 1], 0.0)
    upper = jnp.concatenate([table[:, half:], table[:, :half]], axis=1)
    table = jnp.where(lane == 0, table, upper)
    gg[0, 0] = jnp.concatenate([table, table], axis=1)

    pl.semaphore_wait(barrier, len(others))

    cuts = [pl.ds(p * (half // PIECES), half // PIECES) for p in range(PIECES)]

    def onward(k, p, cut):
        bit = 1
        while bit < lines:
            if bit > k:
                to = k + bit
                remote(
                    xg.at[k, 0, 0, cut], xg.at[to, 0, 0, cut], zx_s.at[to, p], zx_r.at[to, p],
                    peer_z[bit],
                )
                if p == 0:
                    remote(gg.at[k, 0], gg.at[to, 0], zg_s.at[to], zg_r.at[to], peer_z[bit])
            bit *= 2
        remote(xg.at[k, 0, 0, cut], xg.at[k, 0, 1, cut], yx_s.at[k, p], yx_r.at[k, p], peer_y)
        if p == 0:
            remote(gg.at[k, 0], gg.at[k, 1], yg_s.at[k], yg_r.at[k], peer_y)

    for p, cut in enumerate(cuts):
        onward(0, p, cut)

    def from_z(k):
        for p, cut in enumerate(cuts):
            landed(xg.at[k, 0, 0, cut], zx_r.at[k, p])
            if p == 0:
                landed(gg.at[k, 0], zg_r.at[k])
            onward(k, p, cut)
        remote(xg.at[k, 0, 0], xg.at[k, 1, 0], dx_s.at[k, 0], dx_r.at[k, 0], peer_c)

    def from_y(k):
        landed(gg.at[k, 1], yg_r.at[k])
        for p, cut in enumerate(cuts):
            landed(xg.at[k, 0, 1, cut], yx_r.at[k, p])
        remote(xg.at[k, 0, 1], xg.at[k, 1, 1], dx_s.at[k, 1], dx_r.at[k, 1], peer_c)

    def compute(k):
        if k:
            landed(xg.at[k, 1, 0], dx_r.at[k, 0])
        landed(xg.at[k, 1, 1], dx_r.at[k, 1])
        if k == 0:
            weights[0].wait()
            weights[1].wait()
        count = 2 * rows
        x = xg[k].reshape(count, width)
        spot = lax.broadcasted_iota(jnp.int32, gg.shape[2:], 1)
        first, second = gg[k, 0], gg[k, 1]
        mine = lax.broadcasted_iota(jnp.int32, gg.shape[2:], 0) == me
        row_a = jnp.sum(jnp.where(mine, first, 0.0), axis=0, keepdims=True)
        row_b = jnp.sum(jnp.where(mine, second, 0.0), axis=0, keepdims=True)
        at = lax.broadcasted_iota(jnp.int32, (count, count), 0)
        token = (at // rows) * half + at % half
        hit = lax.broadcasted_iota(jnp.int32, (count, count), 1) == token
        column = (at // half) % 2
        gate = jnp.sum(
            jnp.where(hit, jnp.where(column == 0, row_a, row_b), 0.0), axis=1, keepdims=True
        )
        g = jnp.dot(x, wg[...], preferred_element_type=jnp.float32)
        u = jnp.dot(x, wu[...], preferred_element_type=jnp.float32)
        hidden = (g / (1.0 + jnp.exp(-g)) * u * gate).astype(jnp.bfloat16)
        if k == 0:
            weights[2].wait()
        y = jnp.dot(hidden, wd[...], preferred_element_type=jnp.float32)
        po[k] = y.astype(jnp.bfloat16).reshape(2, 2, half, width)
        remote(po.at[k, 1], rd.at[k], rd_s.at[k], rd_r.at[k], peer_c)

    def back_y(k):
        landed(rd.at[k], rd_r.at[k])
        for p, cut in enumerate(cuts):
            total = po[k, 0, 1, cut].astype(jnp.float32) + rd[k, 1, cut].astype(jnp.float32)
            ys[k, cut] = total.astype(jnp.bfloat16)
            remote(ys.at[k, cut], ry.at[k, cut], ry_s.at[k, p], ry_r.at[k, p], peer_y)

    def back_z(k):
        for p, cut in enumerate(cuts):
            landed(ry.at[k, cut], ry_r.at[k, p])
            total = (
                po[k, 0, 0, cut].astype(jnp.float32)
                + rd[k, 0, cut].astype(jnp.float32)
                + ry[k, cut].astype(jnp.float32)
            )
            if k == 0:
                keep[cut, :] = total
            else:
                zs[k, cut] = total.astype(jnp.bfloat16)
                remote(zs.at[k, cut], rz.at[k, cut], rz_s.at[k, p], rz_r.at[k, p], peer_z[k])

    def step(fn, k, low=0):
        if low <= k < lines:
            fn(k)

    from_z(1)
    from_y(0)
    step(from_z, 2)
    for k in range(lines):
        compute(k)
        if k < lines - 1:
            step(back_y, k - 1)
        step(from_y, k + 1)
        step(from_z, k + 3)
        if k == lines - 2:
            back_y(k)
    for k in range(1, lines - 2):
        back_z(k)
    back_y(lines - 1)
    for k in range(max(1, lines - 2), lines):
        back_z(k)
    back_z(0)
    total = keep[...]
    for k in range(1, lines):
        for p, cut in enumerate(cuts):
            landed(rz.at[k, cut], rz_r.at[k, p])
        total = total + rz[k].astype(jnp.float32)
    fin[...] = total.astype(jnp.bfloat16)
    remote(fin, ro, ro_s, ro_r, peer_c)
    out_ref[pl.ds(pl.multiple_of(lane * half, half), half), :] = fin[...]
    landed(ro, ro_r)
    out_ref[pl.ds(pl.multiple_of((1 - lane) * half, half), half), :] = ro[...]
    for copy in sent:
        copy.wait_send()


def dense_device(lines, tokens, routes, gates, norm_gain, w_gate, w_up, w_down):
    rows, width = tokens.shape
    half = rows // 2
    units = w_gate.shape[2]
    experts = lines * 2
    bf16, f32 = jnp.bfloat16, jnp.float32
    dma = pltpu.SemaphoreType.DMA
    cut = dma((lines, PIECES))
    vmem, anywhere = pl.BlockSpec(memory_space=pltpu.VMEM), pl.BlockSpec(memory_space=pl.ANY)
    return pl.pallas_call(
        functools.partial(dense_kernel, lines),
        out_shape=pltpu.VMEM((rows, width), bf16),
        in_specs=[vmem] * 4 + [anywhere] * 3,
        out_specs=vmem,
        scratch_shapes=[
            pltpu.VMEM((width, units), bf16),
            pltpu.VMEM((width, units), bf16),
            pltpu.VMEM((units, width), bf16),
            pltpu.VMEM((lines, 2, 2, half, width), bf16),
            pltpu.VMEM((lines, 2, experts, 2 * rows), f32),
            pltpu.VMEM((lines, 2, 2, half, width), bf16),
            pltpu.VMEM((lines, 2, half, width), bf16),
            pltpu.VMEM((lines, half, width), bf16),
            pltpu.VMEM((lines, half, width), bf16),
            pltpu.VMEM((lines, half, width), bf16),
            pltpu.VMEM((lines, half, width), bf16),
            pltpu.VMEM((half, width), f32),
            pltpu.VMEM((half, width), bf16),
            pltpu.VMEM((half, width), bf16),
            dma((3,)),
            cut, cut, dma((lines,)), dma((lines,)),
            cut, cut, dma((lines,)), dma((lines,)),
            dma((lines, 2)), dma((lines, 2)),
            dma((lines,)), dma((lines,)), cut, cut,
            cut, cut, dma, dma,
        ],
        compiler_params=pltpu.CompilerParams(collective_id=0, has_side_effects=True),
    )(tokens, routes.T, gates.T, norm_gain.reshape(1, width), w_gate, w_up, w_down)


def packed_device(tokens, routes, gates, norm_gain, w_gate, w_up, w_down):
    tok_rows, width = tokens.shape
    top = routes.shape[1]
    ep_count = lax.axis_size("ep")
    tp_count = lax.axis_size("tp")
    capacity = max(2, min(tok_rows, 3 * tok_rows * top // ep_count))
    share = width // tp_count
    lane = lax.axis_index("tp")
    xf = tokens.astype(jnp.float32)
    normed = (xf * lax.rsqrt(jnp.mean(xf * xf, axis=-1, keepdims=True) + EPS) * norm_gain).astype(
        jnp.bfloat16
    )
    flat = routes.reshape(-1)
    onehot = (flat[:, None] == jnp.arange(ep_count, dtype=jnp.int32)[None, :]).astype(jnp.int32)
    earlier = jnp.cumsum(onehot, axis=0) - onehot
    rank = jnp.sum(earlier * onehot, axis=1)
    slot = flat * capacity + rank
    placing = (jnp.arange(ep_count * capacity, dtype=jnp.int32)[:, None] == slot[None, :]).astype(
        jnp.bfloat16
    )
    repeated = jnp.repeat(normed, top, axis=0)
    outgoing = jnp.dot(placing, repeated, preferred_element_type=jnp.float32).astype(jnp.bfloat16)
    outgoing = outgoing.reshape(ep_count, capacity, width)
    mine = lax.dynamic_slice_in_dim(outgoing, lane * share, share, 2)
    full = lax.all_gather(
        lax.all_to_all(mine, "ep", split_axis=0, concat_axis=0, tiled=True),
        "tp",
        axis=2,
        tiled=True,
    )
    sources = full.shape[0]
    items = full.shape[1]
    rows = full.reshape(sources * items, width)
    gate_act = jnp.dot(rows, w_gate[0], preferred_element_type=jnp.float32)
    up_act = jnp.dot(rows, w_up[0], preferred_element_type=jnp.float32)
    hidden = (jax.nn.silu(gate_act) * up_act).astype(jnp.bfloat16)
    partial_value = jnp.dot(hidden, w_down[0], preferred_element_type=jnp.float32).astype(
        jnp.bfloat16
    )
    summed = lax.psum_scatter(
        lax.optimization_barrier(partial_value)
        .astype(jnp.float32)
        .reshape(sources, items, width)
        .astype(jnp.bfloat16),
        "tp",
        scatter_dimension=2,
        tiled=True,
    )
    returned = lax.all_to_all(summed, "ep", split_axis=0, concat_axis=0, tiled=True)
    back = returned.reshape(ep_count * capacity, returned.shape[2])
    picked = jnp.take(back, slot, axis=0).reshape(tok_rows, top, back.shape[1])
    mixed = jnp.sum(gates[:, :, None] * picked.astype(jnp.float32), axis=1).astype(jnp.bfloat16)
    mixed = lax.all_gather(mixed, "tp", axis=1, tiled=True)
    return mixed


def per_device(tokens, routes, gates, norm_gain, w_gate, w_up, w_down):
    rows, width = tokens.shape
    ep_count, tp_count = lax.axis_size("ep"), lax.axis_size("tp")
    lines = ep_count // 2
    whole = 3 * rows * routes.shape[1] // ep_count >= rows
    fits = lines >= 4 and lines & (lines - 1) == 0 and lines * 2 == ep_count and ep_count % 8 == 0
    if whole and fits and tp_count == 2 and rows % 64 == 0 and width % 128 == 0:
        return dense_device(lines, tokens, routes, gates, norm_gain, w_gate, w_up, w_down)
    return packed_device(tokens, routes, gates, norm_gain, w_gate, w_up, w_down)


def solution(mesh):
    return jax.shard_map(
        per_device,
        mesh=mesh,
        in_specs=(
            P(("grp", "ep"), None),
            P(("grp", "ep"), None),
            P(("grp", "ep"), None),
            P(),
            P("ep", None, "tp"),
            P("ep", None, "tp"),
            P("ep", "tp", None),
        ),
        out_specs=P(("grp", "ep"), None),
        check_vma=False,
    )
```
